512 devices in a mesh: sp: 16 (over z), fs: 4 (over y), tp: 8 (over x, core).
Axes of the slice: x: 4, y: 4, z: 16, core: 2. Of those that a mesh axis runs over, the one named last changes fastest.
Arguments:
- tokens: bfloat16 [4, 4096, 2048], P('fs', ('sp', 'tp')), may hold values from -6 to 6
- query_weight: bfloat16 [2048, 2048], P(('sp', 'fs'), 'tp'), may hold values from -0.125 to 0.125
- forget_weight: bfloat16 [2048, 2048], P(('sp', 'fs'), 'tp'), may hold values from -0.125 to 0.125
- value_weight: bfloat16 [2048, 2048], P(('sp', 'fs'), 'tp'), may hold values from -0.125 to 0.125
- convolution_gate_weight: bfloat16 [2048, 1024], P(('sp', 'fs'), 'tp'), may hold values from -0.125 to 0.125
- convolution_multiplier_weight: bfloat16 [2048, 1024], P(('sp', 'fs'), 'tp'), may hold values from -0.125 to 0.125
- convolution_input_weight: bfloat16 [2048, 1024], P(('sp', 'fs'), 'tp'), may hold values from -0.125 to 0.125
- gate_headroom: float32 [2048], P('tp'), may hold values from 2.4414063e-05 to 0.06
- added_log_rate: float32 [4, 16, 4096], P('fs', 'tp', 'sp'), may hold values from -1.6 to 0
- initial_state: float32 [4, 16, 128, 128], P('fs', 'tp'), may hold values from -0.25 to 0.25
- head_norm_gain: float32 [2048], P('tp'), may hold values from 0.1 to 1.9
- convolution_taps: float32 [3, 1024], P(None, 'tp'), may hold values from -3.5 to 3.5
- convolution_bias: float32 [1024], P('tp'), may hold values from -4 to 4
- recurrence_output_weight: bfloat16 [2048, 2048], P('tp', ('sp', 'fs')), may hold values from -0.109375 to 0.109375
- convolution_output_weight: bfloat16 [1024, 2048], P('tp', ('sp', 'fs')), may hold values from -0.109375 to 0.109375
Outputs:
- mixed: bfloat16 [4, 4096, 2048], P('fs', ('sp', 'tp'))
The draws below stay inside these ranges and needn't reach their ends.
All inputs are finite; a program needn't handle non-finite values.
Results may differ from the reference program's by a relative error of at most 0.018.
Values may be sent and summed in bfloat16 or wider, within the bound.
A program may use at most 64 MiB of HBM per device.

```python
import jax
import jax.numpy as jnp
from jax import lax

D = 2048
RECURRENCE_HEADS = 16
DK = 128
CV = 1024
KW = 3
BLOCK_POSITIONS = 64
TOK = 256
HK = 2048
SEQ = 4096
BATCH = 4
N_TP = 8


def draw_gate_headroom(key, part):
    key_order, key_slow, key_fast = jax.random.split(jax.random.fold_in(key, 11), 3)
    head_order = jax.random.permutation(key_order, RECURRENCE_HEADS)
    slow_count = RECURRENCE_HEADS // 2
    slow_low = 0.25
    slow_high = 1.0
    slow_head = head_order < slow_count
    unit_slow = jax.random.uniform(key_slow, (RECURRENCE_HEADS, DK), jnp.float32)
    unit_fast = jax.random.uniform(key_fast, (RECURRENCE_HEADS, DK), jnp.float32)
    slow_gap = jnp.exp(jnp.log(slow_low) + unit_slow * (jnp.log(slow_high) - jnp.log(slow_low))) / SEQ
    fast_gap = jnp.exp(jnp.log(0.02) + unit_fast * (jnp.log(0.06) - jnp.log(0.02)))
    return jnp.where(slow_head[:, None], slow_gap, fast_gap).reshape(RECURRENCE_HEADS * DK).astype(jnp.float32)


def draw_added_log_rate(key, part):
    key_rate, key_spot, key_kept = jax.random.split(jax.random.fold_in(key, 23), 3)
    span_count = SEQ // TOK
    rate_low = 0.25
    rate_high = 1.0
    block_unit = jax.random.uniform(key_rate, (BATCH, 1, span_count, 1), jnp.float32)
    block_rate = jnp.exp(jnp.log(rate_low) + block_unit * (jnp.log(rate_high) - jnp.log(rate_low))) / SEQ
    stable_part = jnp.broadcast_to(-block_rate, (BATCH, RECURRENCE_HEADS, span_count, TOK)).reshape(BATCH, RECURRENCE_HEADS, SEQ)
    spots = jax.random.randint(key_spot, (BATCH, RECURRENCE_HEADS, 2), 0, SEQ)
    retained_fraction = jax.random.uniform(key_kept, (BATCH, RECURRENCE_HEADS, 2), jnp.float32, minval=0.5, maxval=0.8)
    at_location = jnp.arange(SEQ)[None, None, :, None] == spots[:, :, None, :]
    extra_log_rate = jnp.sum(jnp.where(at_location, jnp.log(retained_fraction)[:, :, None, :], 0.0), axis=-1)
    return (stable_part + extra_log_rate).astype(jnp.float32)


def block_scale(own_key, extent, cuts, low, largest):
    loudness, own = 1.0, jax.random.fold_in(own_key, 6)
    for dim, shards_of in cuts:
        draws = jnp.exp(jax.random.uniform(jax.random.fold_in(own, dim), (shards_of,), jnp.float32, low / len(cuts), largest / len(cuts)))
        loudness = loudness * jnp.repeat(draws, extent[dim] // shards_of).reshape([-1 if axis == dim else 1 for axis in range(len(extent))])
    return loudness


def bell_draw(key, dims, scale, limit, cuts=(), kind=jnp.bfloat16):
    gain = block_scale(key, dims, cuts, -0.22, 0.18) if cuts else 1.0
    entries = jax.random.normal(key, dims, jnp.float32) * scale * gain
    return jnp.minimum(jnp.maximum(entries, -limit), limit).astype(kind)


def setup_inputs(seed: int = 0) -> dict:
    streams_of = jax.random.split(jax.random.key(seed), 16)
    tokens = bell_draw(streams_of[0], (BATCH, SEQ, D), 1.0, 6.0, ((0, 4), (1, 128)))
    query_weight = bell_draw(streams_of[1], (D, HK), D ** -0.5, 0.125, ((0, 64), (1, 8)))
    forget_weight = bell_draw(streams_of[2], (D, HK), D ** -0.5, 0.125, ((0, 64), (1, 8)))
    value_weight = bell_draw(streams_of[3], (D, HK), D ** -0.5, 0.125, ((0, 64), (1, 8)))
    convolution_gate_weight = bell_draw(streams_of[4], (D, CV), D ** -0.5, 0.125, ((0, 64), (1, 8)))
    convolution_multiplier_weight = bell_draw(streams_of[5], (D, CV), D ** -0.5, 0.125, ((0, 64), (1, 8)))
    convolution_input_weight = bell_draw(streams_of[6], (D, CV), D ** -0.5, 0.125, ((0, 64), (1, 8)))
    gate_headroom = draw_gate_headroom(jax.random.fold_in(streams_of[15], 71), 0)
    added_log_rate = draw_added_log_rate(jax.random.fold_in(streams_of[15], 71), 0)
    initial_state = bell_draw(streams_of[9], (BATCH, RECURRENCE_HEADS, DK, DK), (SEQ ** -0.5), 0.25, ((0, 4), (1, 8)), jnp.float32)
    head_norm_gain = jnp.clip(1.0 + 0.18 * jax.random.normal(streams_of[10], (HK,), jnp.float32), 0.1, 1.9)
    convolution_taps = bell_draw(streams_of[11], (KW, CV), KW ** -0.5, 3.5, ((1, 8),), jnp.float32)
    convolution_bias = bell_draw(streams_of[12], (CV,), 1.0, 4.0, ((0, 8),), jnp.float32)
    recurrence_output_weight = bell_draw(streams_of[13], (HK, D), (HK + CV) ** -0.5, 0.109375, ((0, 8), (1, 64)))
    convolution_output_weight = bell_draw(streams_of[14], (CV, D), (HK + CV) ** -0.5, 0.109375, ((0, 8), (1, 64)))
    return {"tokens": tokens, "query_weight": query_weight, "forget_weight": forget_weight, "value_weight": value_weight, "convolution_gate_weight": convolution_gate_weight, "convolution_multiplier_weight": convolution_multiplier_weight, "convolution_input_weight": convolution_input_weight, "gate_headroom": gate_headroom, "added_log_rate": added_log_rate, "initial_state": initial_state, "head_norm_gain": head_norm_gain, "convolution_taps": convolution_taps, "convolution_bias": convolution_bias, "recurrence_output_weight": recurrence_output_weight, "convolution_output_weight": convolution_output_weight}


def project(sequence_rows, weight):
    return jnp.dot(sequence_rows, weight, preferred_element_type=jnp.float32).astype(jnp.bfloat16)

def to_blocks(values, number_of_blocks):
    return jnp.transpose(values.reshape(number_of_blocks, BLOCK_POSITIONS, RECURRENCE_HEADS, DK), (2, 0, 1, 3))

def gated_recurrence(query_vectors, forget_logits, value_vectors, gate_headroom, extra_rates, opening_state):
    length = query_vectors.shape[0]
    number_of_blocks = length // BLOCK_POSITIONS
    query_scaled = to_blocks(query_vectors.astype(jnp.float32), number_of_blocks) * DK ** (-0.5)
    gated_key = to_blocks(gate_headroom[None, :] * jax.nn.sigmoid(-forget_logits.astype(jnp.float32)), number_of_blocks)
    forget_log_rate = jnp.log1p(-gated_key) + extra_rates.reshape(RECURRENCE_HEADS, number_of_blocks, BLOCK_POSITIONS)[..., None]
    values = to_blocks(value_vectors.astype(jnp.float32), number_of_blocks)
    cumulative = jnp.cumsum(forget_log_rate, axis=2)
    query_decayed = query_scaled * jnp.exp(cumulative)
    key_decayed = gated_key * jnp.exp(-cumulative)
    scores = jnp.einsum('hnik,hnjk->hnij', query_decayed, key_decayed, precision=lax.Precision.HIGHEST)
    causal = jnp.tril(jnp.ones((BLOCK_POSITIONS, BLOCK_POSITIONS), dtype=bool))
    scores = jnp.where(causal, scores, 0.0)
    within = jnp.einsum('hnij,hnjv->hniv', scores, values, precision=lax.Precision.HIGHEST)
    final_log = cumulative[:, :, -1:, :]
    contrib = jnp.einsum('hnck,hncv->hnkv', gated_key * jnp.exp(final_log - cumulative), values, precision=lax.Precision.HIGHEST)
    decays = jnp.exp(final_log[:, :, 0, :])

    def advance(current, block_pair):
        return (block_pair[0][..., None] * current + block_pair[1], current)
    _, entering = lax.scan(advance, opening_state, (jnp.moveaxis(decays, 1, 0), jnp.moveaxis(contrib, 1, 0)))
    entering = jnp.moveaxis(entering, 0, 1)
    carried_term = jnp.einsum('hnck,hnkv->hncv', query_decayed, entering, precision=lax.Precision.HIGHEST)
    return jnp.transpose(within + carried_term, (1, 2, 0, 3)).reshape(length, RECURRENCE_HEADS, DK)

def reference(tokens, query_weight, forget_weight, value_weight, convolution_gate_weight, convolution_multiplier_weight, convolution_input_weight, gate_headroom, added_log_rate, initial_state, head_norm_gain, convolution_taps, convolution_bias, recurrence_output_weight, convolution_output_weight):

    def single_sequence(input_rows):
        sequence_rows, extra_rates, opening_state = input_rows
        length = sequence_rows.shape[0]
        query_vectors = project(sequence_rows, query_weight)
        forget_logits = project(sequence_rows, forget_weight)
        value_vectors = project(sequence_rows, value_weight)
        conv_gate = project(sequence_rows, convolution_gate_weight)
        conv_mult = project(sequence_rows, convolution_multiplier_weight)
        conv_input = project(sequence_rows, convolution_input_weight)
        recurrence_unnormed = gated_recurrence(query_vectors, forget_logits, value_vectors, gate_headroom, extra_rates, opening_state)
        mean_square = lax.optimization_barrier(jnp.mean(recurrence_unnormed * recurrence_unnormed, axis=-1, keepdims=True))
        rec_out = recurrence_unnormed * lax.rsqrt(mean_square + 1e-06) * head_norm_gain.reshape(RECURRENCE_HEADS, DK)
        rec_out = rec_out.reshape(length, HK).astype(jnp.bfloat16)
        conv_prod = conv_mult.astype(jnp.float32) * conv_input.astype(jnp.float32)
        padded = jnp.concatenate([jnp.zeros((KW - 1, CV), jnp.float32), conv_prod], axis=0)
        conv_y = jnp.broadcast_to(convolution_bias[None, :], (length, CV))
        for j in range(KW):
            conv_y = conv_y + convolution_taps[j][None, :] * padded[j:j + length]
        conv_out = (conv_gate.astype(jnp.float32) * conv_y).astype(jnp.bfloat16)
        rec_group = HK // N_TP
        conv_group = CV // N_TP
        running = jnp.zeros((length, D), jnp.float32)
        for g in range(N_TP):
            partial_value = jnp.dot(rec_out[:, g * rec_group:(g + 1) * rec_group], recurrence_output_weight[g * rec_group:(g + 1) * rec_group], preferred_element_type=jnp.float32)
            partial_value = partial_value + jnp.dot(conv_out[:, g * conv_group:(g + 1) * conv_group], convolution_output_weight[g * conv_group:(g + 1) * conv_group], preferred_element_type=jnp.float32)
            running = running + lax.optimization_barrier(partial_value.astype(jnp.bfloat16)).astype(jnp.float32)
        return running.astype(jnp.bfloat16)
    return lax.map(single_sequence, (tokens, added_log_rate, initial_state))
```

```python
import functools

import jax
import jax.numpy as jnp
from jax import lax
from jax.experimental import pallas as pl
from jax.experimental.pallas import tpu as pltpu
from jax.sharding import PartitionSpec as P

F32 = jnp.float32
BF16 = jnp.bfloat16
MESH = pl.DeviceIdType.MESH
DK = 128
BLOCK = 64
NX = 4
NY = 4


def dot(a, b):
    return lax.dot_general(a, b, (((1,), (0,)), ((), ())), preferred_element_type=F32)


def dot_nt(a, b):
    return lax.dot_general(a, b, (((1,), (1,)), ((), ())), preferred_element_type=F32)


def dot_tn(a, b):
    return lax.dot_general(a, b, (((0,), (0,)), ((), ())), preferred_element_type=F32)


def three_words(a):
    high = a.astype(BF16)
    rest = a - high.astype(F32)
    middle = rest.astype(BF16)
    low = (rest - middle.astype(F32)).astype(BF16)
    return high, middle, low


def layer(
    nz,
    tok,
    wq,
    wf,
    wv,
    wg,
    wm,
    wi,
    small,
    s0,
    wot,
    out,
    wbuf,
    wob,
    xbuf,
    sta,
    stb,
    spbuf,
    s0buf,
    sbuf,
    vbuf,
    kgbuf,
    cumbuf,
    offbuf,
    qbuf,
    recbuf,
    qbbuf,
    gatebuf,
    ext,
    halo,
    actr,
    actc,
    abuf,
    pbuf,
    rbuf,
    ssem,
    wsem,
    spsem,
    s0sem,
    ringw,
    rings,
    onesem,
    wysem,
):
    z = lax.axis_index("sp")
    y = lax.axis_index("fs")
    t = lax.axis_index("tp")
    x = t // 2
    c = t % 2
    y2 = y // 2
    y1 = y % 2
    other = 1 - c
    width = nz * NY * 32

    def dev(z_, y_, x_, c_):
        return {"sp": z_, "fs": y_, "tp": 2 * x_ + c_}

    partner = dev(z, y, x, other)
    up = dev((z + 1) % nz, y, x, c)
    down = dev((z + nz - 1) % nz, y, x, c)

    used = [0]
    pending = []

    def send(src, dst, rsem, to, local=None):
        sem = ssem.at[used[0]]
        used[0] += 1
        copy = pltpu.make_async_remote_copy(src, dst, sem, rsem, device_id=to, device_id_type=MESH)
        if local is None:
            copy.start()
            pending.append(copy.wait_send)
            return
        here = pltpu.make_async_copy(src, dst, rsem)
        away = jnp.logical_not(local)

        @pl.when(away)
        def _():
            copy.start()

        @pl.when(local)
        def _():
            here.start()

        def finish():
            @pl.when(away)
            def _():
                copy.wait_send()

        pending.append(finish)

    def drain(ref, sem):
        pltpu.make_async_copy(ref, ref, sem).wait()

    def ring(chunks, last_up, sems, arrived, hooks):
        half = nz // 2

        def carries(direction, i, k):
            return k < half or (i in last_up) == (direction == 0)

        def pass_on(k, i, direction, zi):
            if carries(direction, i, k + 1):
                ref = chunks[i](zi)
                send(ref, ref, sems.at[direction, k, i], up if direction == 0 else down)

        for i in range(len(chunks)):
            for direction in (0, 1):
                pass_on(0, i, direction, z)
            arrived(i, z)
        hooks(0)
        for k in range(1, half + 1):
            for i in range(len(chunks)):
                for direction in (0, 1):
                    if not carries(direction, i, k):
                        continue
                    zi = (z + nz - k) % nz if direction == 0 else (z + k) % nz
                    drain(chunks[i](zi), sems.at[direction, k - 1, i])
                    if k < half:
                        pass_on(k, i, direction, zi)
                    arrived(i, zi)
            hooks(k)

    STA, STB, XS, WD, WOD, WOWN, HALO, ACT, RS = range(9)

    own_out = pltpu.make_async_copy(wot, wob.at[c, z, y], onesem.at[WOWN])
    own_out.start()
    pltpu.make_async_copy(tok.at[pl.ds(0, 16)], sta.at[x], onesem.at[STA]).start()
    pltpu.make_async_copy(tok.at[pl.ds(16, 16)], stb.at[y], onesem.at[STB]).start()

    barrier = pltpu.get_barrier_semaphore()
    greeted = [partner, up, down]
    for d in range(1, NX):
        for core in (0, 1):
            greeted.append(dev(z, y, (x + d) % NX, core))
    for d in range(1, NY):
        for core in (0, 1):
            greeted.append(dev(z, (y + d) % NY, x, core))
    for peer in greeted:
        pl.semaphore_signal(barrier, inc=1, device_id=peer, device_id_type=MESH)
    pl.semaphore_wait(barrier, len(greeted))

    row = (z * NY + y) * 32
    for j in (0, 1):
        to = dev(z, 2 * c + j, x, y2)
        local = jnp.logical_and(y2 == c, y1 == j)
        pieces = [(wf, j * DK), (wv, j * DK), (wq, j * DK), (wg, 0), (wm, 0), (wi, 0)]
        for m, (ref, at) in enumerate(pieces):
            send(
                ref.at[:, pl.ds(at, DK)],
                wbuf.at[pl.ds(row, 32), pl.ds(m * DK, DK)],
                wsem.at[y1],
                to,
                local,
            )
    for d in range(1, NX):
        send(
            tok.at[pl.ds(0, 16)], sta.at[x], onesem.at[STA], dev(z, y, (x + d) % NX, c)
        )
        send(
            tok.at[pl.ds(16, 16)], stb.at[y], onesem.at[STB], dev(z, (y + d) % NY, x, c)
        )
    for j in (0, 1):
        to = dev(z, 2 * c + j, x, y2)
        local = jnp.logical_and(y2 == c, y1 == j)
        send(small.at[j], spbuf.at[y1], spsem.at[y1], to, local)
        send(s0.at[j], s0buf.at[y1], s0sem.at[y1], to, local)

    own_out.wait()
    for i in (0, 1):
        drain(wbuf.at[pl.ds(z * 128 + c * 64 + i * 32, 32)], wsem.at[i])

    def weight_chunk(i):
        return lambda zi: wbuf.at[pl.ds(pl.multiple_of(zi * 128 + c * 64 + i * 32, 32), 32)]

    def out_chunk(zi):
        return wob.at[c, zi, y]

    def weight_arrived(i, zi):
        if i < 2:
            ref = weight_chunk(i)(zi)
            send(ref, ref, onesem.at[WD], partner)

    def spread_tokens(k):
        if k != 1:
            return
        drain(sta, onesem.at[STA])
        for d in range(1, NY):
            send(sta, xbuf.at[y1, :, c, 0], onesem.at[XS], dev(z, (y + d) % NY, x, y2))
        send(sta, xbuf.at[y1, :, c, 0], onesem.at[XS], dev(z, y, x, y2), y2 == c)
        drain(stb, onesem.at[STB])
        for d in range(1, NX):
            for core in (0, 1):
                send(
                    stb.at[pl.ds(2 * core, 2)],
                    xbuf.at[:, x, c, 1],
                    onesem.at[XS],
                    dev(z, y, (x + d) % NX, core),
                )
        send(stb.at[pl.ds(2 * other, 2)], xbuf.at[:, x, c, 1], onesem.at[XS], partner)
        pltpu.make_async_copy(
            stb.at[pl.ds(2 * c, 2)], xbuf.at[:, x, c, 1], onesem.at[XS]
        ).start()

    ring([weight_chunk(0), weight_chunk(1), out_chunk], (0,), ringw, weight_arrived, spread_tokens)

    for d in range(1, NY):
        send(wob.at[c, :, y], wob.at[c, :, y], wysem.at[d - 1], dev(z, (y + d) % NY, x, c))
    send(wob.at[c, :, y], wob.at[c, :, y], onesem.at[WOD], partner)

    drain(xbuf, onesem.at[XS])
    drain(wbuf.at[pl.ds(0, width // 2)], onesem.at[WD])
    for i in (0, 1):
        drain(spbuf.at[i], spsem.at[i])

    rows = lax.broadcasted_iota(jnp.int32, (256, 256), 0)
    cols = lax.broadcasted_iota(jnp.int32, (256, 256), 1)
    causal = jnp.logical_and(rows // BLOCK == cols // BLOCK, cols <= rows)
    lower = jnp.where(causal, 1.0, 0.0).astype(BF16)
    word = lax.broadcasted_iota(jnp.int32, (16, DK), 0)

    def tokens_of(s):
        return xbuf[s].reshape(256, width)

    for s in (0, 1):
        fv = dot(tokens_of(s), wbuf[:, 0 : 2 * DK])
        forget = fv[:, :DK].astype(BF16).astype(F32)
        value = fv[:, DK:].astype(BF16)
        key_gate = spbuf[s, 0:1, :] * jax.nn.sigmoid(-forget)
        rates = jnp.concatenate(
            [
                jnp.transpose(jnp.broadcast_to(spbuf[s, 6 + h : 7 + h, :], (DK, DK)))
                for h in (0, 1)
            ],
            axis=0,
        )
        log_forget = jnp.log1p(-key_gate) + rates
        sums = dot(lower, jnp.concatenate(three_words(log_forget), axis=1))
        cum = sums[:, :DK] + sums[:, DK : 2 * DK] + sums[:, 2 * DK :]
        total = jnp.zeros((1, DK), F32)
        offsets = []
        for n in range(4):
            offsets.append(jnp.broadcast_to(total, (BLOCK, DK)))
            total = total + cum[n * BLOCK + BLOCK - 1 : n * BLOCK + BLOCK, :]
        offset = jnp.concatenate(offsets, axis=0)
        kept = (key_gate * jnp.exp(total - (cum + offset))).astype(BF16)
        sbuf[z, s, 0:DK, :] = dot_tn(value, kept).astype(BF16)
        high, middle, low = [
            jnp.broadcast_to(w.astype(F32), (16, DK)) for w in three_words(jnp.exp(total))
        ]
        words = jnp.where(word == 0, high, jnp.where(word == 1, middle, low))
        sbuf[z, s, DK : DK + 16, :] = words.astype(BF16)
        vbuf[s] = value
        kgbuf[s] = key_gate
        cumbuf[s] = cum
        offbuf[s] = offset

    def state_chunk(s):
        return lambda zi: sbuf.at[zi, s]

    def query_work():
        for s in (0, 1):
            q = dot(tokens_of(s), wbuf[:, 2 * DK : 3 * DK]).astype(BF16)
            qbuf[s] = q.astype(F32) * DK ** (-0.5)

    def conv_work():
        projected = dot(tokens_of(y1), wbuf[:, 3 * DK : 6 * DK]).astype(BF16).astype(F32)
        gatebuf[...] = projected[:, :DK]
        ext[8:264, :] = projected[:, DK : 2 * DK] * projected[:, 2 * DK :]
        send(ext.at[pl.ds(256, 8)], halo, onesem.at[HALO], up)

    def block_work(s):
        cum = cumbuf[s]
        key_gate = kgbuf[s]
        value = vbuf[s]
        decayed = qbuf[s] * jnp.exp(cum)
        qbbuf[s] = (decayed * jnp.exp(offbuf[s])).astype(BF16)
        queries = decayed.astype(BF16)
        keys = (key_gate * jnp.exp(-cum)).astype(BF16)
        scores = jnp.where(causal, dot_nt(queries, keys), 0.0).astype(BF16)
        recbuf[s] = dot(scores, value)
        entering = None
        for n in range(4):
            at = slice(n * BLOCK, n * BLOCK + BLOCK)
            final = cum[n * BLOCK + BLOCK - 1 : n * BLOCK + BLOCK, :]
            if entering is not None:
                recbuf[s, at, :] += dot_nt(queries[at], entering.astype(BF16))
            if n < 3:
                kept = (key_gate[at] * jnp.exp(final - cum[at])).astype(BF16)
                here = dot_tn(value[at], kept)
                entering = here if entering is None else jnp.exp(final) * entering + here

    def conv_finish():
        drain(halo, onesem.at[HALO])
        ext[0:8, :] = jnp.where(z == 0, 0.0, halo[...])
        conv = jnp.broadcast_to(spbuf[0, 5:6, :], (256, DK))
        for j in range(3):
            conv = conv + spbuf[0, 2 + j : 3 + j, :] * ext[6 + j : 262 + j, :]
        actc[...] = (gatebuf[...] * conv).astype(BF16).reshape(NX, 2, 32, DK)
        for core in (0, 1):
            send(
                actc.at[:, core],
                abuf.at[y2 * 3 + 2],
                onesem.at[ACT],
                dev(z, 2 * c + y1, x, core),
                jnp.logical_and(y2 == c, c == core),
            )

    def out_weights(d):
        ref = wob.at[c, :, (y + NY - d) % NY]
        drain(ref, wysem.at[d - 1])
        send(ref, ref, onesem.at[WOD], partner)

    def meanwhile(k):
        if k == 0:
            query_work()
        elif k == 1:
            conv_work()
        elif k == 2:
            block_work(0)
        elif k == 3:
            block_work(1)
        elif k == 4:
            conv_finish()

    ring([state_chunk(0), state_chunk(1)], (0,), rings, lambda i, zi: None, meanwhile)

    for d in range(1, NY):
        out_weights(d)

    for s in (0, 1):
        drain(s0buf.at[s], s0sem.at[s])
        carried = jnp.transpose(s0buf[s])
        for j in range(nz - 1):
            words = sbuf[j, s, DK : DK + 16, :].astype(F32)
            decay = words[0:1] + words[1:2] + words[2:3]
            later = decay * carried + sbuf[j, s, 0:DK, :].astype(F32)
            carried = jnp.where(j < z, later, carried)
        raw = recbuf[s] + dot_nt(qbbuf[s], carried.astype(BF16))
        mean_square = jnp.mean(raw * raw, axis=-1, keepdims=True)
        rec = raw * lax.rsqrt(mean_square + 1e-06) * spbuf[s, 1:2, :]
        actr[s] = rec.astype(BF16).reshape(NX, 2, 32, DK)
        for core in (0, 1):
            send(
                actr.at[s, :, core],
                abuf.at[y2 * 3 + y1],
                onesem.at[ACT],
                dev(z, 2 * c + s, x, core),
                jnp.logical_and(y == 2 * c + s, c == core),
            )

    drain(wob.at[other], onesem.at[WOD])
    drain(abuf, onesem.at[ACT])
    acts = [
        jnp.concatenate([abuf[3 * g + m].reshape(128, DK) for m in range(3)], axis=1)
        for g in (0, 1)
    ]
    for part in range(nz // 4):
        at = slice(4 * part, 4 * part + 4)
        partial = dot_nt(acts[0], wob[0, at].reshape(512, 3 * DK)) + dot_nt(
            acts[1], wob[1, at].reshape(512, 3 * DK)
        )
        pbuf[:, :, 512 * part : 512 * part + 512] = partial.astype(BF16).reshape(NX, 32, 512)
        for d in (2, 1, 3):
            to = (x + d) % NX
            cut = pl.ds(512 * part, 512)
            send(pbuf.at[to, :, cut], rbuf.at[x, :, cut], onesem.at[RS], dev(z, y, to, c))
    total = pbuf[x].astype(F32)
    drain(rbuf.at[pl.ds(0, NX - 1)], onesem.at[RS])
    for d in range(1, NX):
        total = total + rbuf[(x + d) % NX].astype(F32)
    out[...] = total.astype(BF16)
    for finish in pending:
        finish()


SENDS = 400


def shards(
    tokens,
    query_weight,
    forget_weight,
    value_weight,
    convolution_gate_weight,
    convolution_multiplier_weight,
    convolution_input_weight,
    gate_headroom,
    added_log_rate,
    initial_state,
    head_norm_gain,
    convolution_taps,
    convolution_bias,
    recurrence_output_weight,
    convolution_output_weight,
):
    nz = lax.axis_size("sp")
    width = tokens.shape[-1]

    def both(a):
        return jnp.broadcast_to(a[None], (2, *a.shape))

    small = jnp.concatenate(
        [
            gate_headroom.reshape(2, 1, DK),
            head_norm_gain.reshape(2, 1, DK),
            both(convolution_taps),
            both(convolution_bias.reshape(1, DK)),
            added_log_rate[0].reshape(2, 2, DK),
        ],
        axis=1,
    )
    out_weights = jnp.concatenate(
        [recurrence_output_weight.T, convolution_output_weight.T], axis=1
    )
    vmem = pl.BlockSpec(memory_space=pltpu.VMEM)
    call = pl.pallas_call(
        functools.partial(layer, nz),
        out_shape=jax.ShapeDtypeStruct((32, width), BF16),
        in_specs=[vmem] * 10,
        out_specs=vmem,
        scratch_shapes=[
            pltpu.VMEM((width, 6 * DK), BF16),
            pltpu.VMEM((2, nz, NY, 32, 3 * DK), BF16),
            pltpu.VMEM((2, NX, 2, 2, 16, width), BF16),
            pltpu.VMEM((NX, 16, width), BF16),
            pltpu.VMEM((NY, 16, width), BF16),
            pltpu.VMEM((2, 8, DK), F32),
            pltpu.VMEM((2, DK, DK), F32),
            pltpu.VMEM((nz, 2, DK + 16, DK), BF16),
            pltpu.VMEM((2, 256, DK), BF16),
            pltpu.VMEM((2, 256, DK), F32),
            pltpu.VMEM((2, 256, DK), F32),
            pltpu.VMEM((2, 256, DK), F32),
            pltpu.VMEM((2, 256, DK), F32),
            pltpu.VMEM((2, 256, DK), F32),
            pltpu.VMEM((2, 256, DK), BF16),
            pltpu.VMEM((256, DK), F32),
            pltpu.VMEM((264, DK), F32),
            pltpu.VMEM((8, DK), F32),
            pltpu.VMEM((2, NX, 2, 32, DK), BF16),
            pltpu.VMEM((NX, 2, 32, DK), BF16),
            pltpu.VMEM((6, NX, 32, DK), BF16),
            pltpu.VMEM((NX, 32, width), BF16),
            pltpu.VMEM((NX, 32, width), BF16),
            pltpu.SemaphoreType.DMA((SENDS,)),
            pltpu.SemaphoreType.DMA((2,)),
            pltpu.SemaphoreType.DMA((2,)),
            pltpu.SemaphoreType.DMA((2,)),
            pltpu.SemaphoreType.DMA((2, nz // 2, 3)),
            pltpu.SemaphoreType.DMA((2, nz // 2, 2)),
            pltpu.SemaphoreType.DMA((9,)),
            pltpu.SemaphoreType.DMA((NY - 1,)),
        ],
        compiler_params=pltpu.CompilerParams(collective_id=0, has_side_effects=True),
    )
    mixed = call(
        tokens[0],
        query_weight,
        forget_weight,
        value_weight,
        convolution_gate_weight,
        convolution_multiplier_weight,
        convolution_input_weight,
        small,
        initial_state[0],
        out_weights,
    )
    return mixed[None]


def solution(mesh):
    in_specs = (
        P("fs", ("sp", "tp"), None),
        P(("sp", "fs"), "tp"),
        P(("sp", "fs"), "tp"),
        P(("sp", "fs"), "tp"),
        P(("sp", "fs"), "tp"),
        P(("sp", "fs"), "tp"),
        P(("sp", "fs"), "tp"),
        P("tp"),
        P("fs", "tp", "sp"),
        P("fs", "tp", None, None),
        P("tp"),
        P(None, "tp"),
        P("tp"),
        P("tp", ("sp", "fs")),
        P("tp", ("sp", "fs")),
    )
    out_specs = P("fs", ("sp", "tp"), None)
    return jax.shard_map(shards, mesh=mesh, in_specs=in_specs, out_specs=out_specs, check_vma=False)
```
